32 devices in a mesh: gr: 2 (over x), sp: 8 (over z, y), tp: 2 (over core).
Axes of the slice: x: 2, y: 2, z: 4, core: 2. Of those that a mesh axis runs over, the one named last changes fastest.
Arguments:
- tokens: bfloat16 [8, 1536, 4096], P('gr', 'sp', 'tp'), may hold values from -6.5 to 6.5
- first_token_input: bfloat16 [8, 4096], P('gr', 'sp'), may hold values from -6 to 6
- forget_weight: bfloat16 [4096, 4096], P(None, 'tp'), may hold values from -0.1171875 to 0.1171875
- value_weight: bfloat16 [4096, 4096], P(None, 'tp'), may hold values from -0.375 to 0.375
- query_weight: bfloat16 [4096, 4096], P('sp', 'tp'), may hold values from -0.09375 to 0.09375
- output_gate_weight: bfloat16 [4096, 4096], P('sp', 'tp'), may hold values from -0.09375 to 0.09375
- forget_bound_slack: float32 [4096], P('tp'), may hold values from 0.00032552083 to 0.8, as said below
- additional_damping_exponent: float32 [8, 1536, 32], P('gr', 'sp', 'tp'), may hold values from -2.2 to 0, as said below
- read_norm_scale: float32 [128], replicated, may hold values from 0.1 to 1.9
Outputs:
- cache: bfloat16 [8, 32, 128, 128], P('gr', 'tp', 'sp')
- first_read: bfloat16 [8, 4096], P('gr', 'tp')
The draws below stay inside these ranges and needn't reach their ends.
Inputs may be any that keep to these rules, and one draw needn't show every extreme that they name: `forget_bound_slack`: positive gaps, one per channel. `additional_damping_exponent`: non-positive log-decays.
All inputs are finite; a program needn't handle non-finite values.
Results may differ from the reference program's by a relative error of at most 0.018.
Values may be sent and summed in bfloat16 or wider, within the bound.
A program may use at most 128 MiB of HBM per device.

```python
import math
import jax
import jax.numpy as jnp
from jax import lax

D = 4096
HEADS = 32
ATTENTION_SPAN = 128
HW = 4096
LEN = 1536
SEQS_ALL = 8


def shared_direction(key):
    signs = jax.random.randint(jax.random.fold_in(key, 101), (D,), 0, 2)
    return (signs * 2 - 1).astype(jnp.float32)


def draw_tokens(key, part):
    direction = shared_direction(key)
    base_key, coef_key = jax.random.split(jax.random.fold_in(key, 31))
    base = jnp.clip(jax.random.normal(base_key, (SEQS_ALL, LEN, D), jnp.float32), -6.0, 6.0)
    coef = jax.random.uniform(coef_key, (SEQS_ALL, 16, 1), jnp.float32, 0.0, 1.5)
    coef = jnp.repeat(coef, LEN // 16, axis=1)
    return (base + coef * 0.3 * direction[None, None, :]).astype(jnp.bfloat16)


def draw_forget_weight(key, part):
    direction = shared_direction(key)
    base_key = jax.random.fold_in(key, 43)
    spread = 1.0 / math.sqrt(D)
    base = jnp.clip(jax.random.normal(base_key, (D, HW), jnp.float32), -6.0, 6.0) * spread
    return (base + 11.0 / D * direction[:, None]).astype(jnp.bfloat16)


def draw_forget_bound_slack(key, part):
    heads_key, jitter_key = jax.random.split(jax.random.fold_in(key, 11))
    share = 0.5
    slow = jax.random.uniform(heads_key, (HEADS,), jnp.float32) < share
    quick = min(0.4, max(0.05, 16.0 / LEN))
    base = jnp.where(slow, 1.0 / LEN, quick)
    jitter = jnp.exp(jax.random.uniform(jitter_key, (HEADS, ATTENTION_SPAN), jnp.float32, -0.69, 0.69))
    return (base[:, None] * jitter).reshape(HEADS * ATTENTION_SPAN).astype(jnp.float32)


def draw_additional_damping_exponent(key, part):
    rate_key, place_key, size_key = jax.random.split(jax.random.fold_in(key, 23), 3)
    rates = jnp.exp(jax.random.uniform(rate_key, (SEQS_ALL, 16, HEADS), jnp.float32, math.log(0.1), 0.0)) / LEN
    rates = jnp.repeat(rates, LEN // 16, axis=1)
    places = jax.random.randint(place_key, (SEQS_ALL, 3), 0, LEN)
    positions = jnp.arange(LEN, dtype=jnp.int32)
    hits = jnp.sum((positions[None, :, None] == places[:, None, :]).astype(jnp.float32), axis=2)
    strength = jax.random.uniform(size_key, (SEQS_ALL, 1, HEADS), jnp.float32, 0.22, 0.69)
    return (-rates - hits[:, :, None] * strength).astype(jnp.float32)


def block_levels(stream_key, shape, cuts, low, top_value):
    def one(dim, blocks):
        steps = jax.random.uniform(jax.random.fold_in(jax.random.fold_in(stream_key, 6), dim), (blocks,), jnp.float32, low / len(cuts), top_value / len(cuts))
        return jnp.repeat(jnp.exp(steps), shape[dim] // blocks).reshape((-1,) + (1,) * (len(shape) - dim - 1))

    level = one(*cuts[0])
    for cut in cuts[1:]:
        level = level * one(*cut)
    return level


def noise(own_key, shape, width, limit, pieces=(), held_as=jnp.bfloat16):
    result = jax.random.normal(own_key, shape, jnp.float32) * width
    if len(pieces) > 0:
        result = block_levels(own_key, shape, pieces, -0.22, 0.18) * result
    return jnp.clip(result, min=-limit, max=limit).astype(held_as)


def setup_inputs(seed: int = 0) -> dict:
    splits = jax.random.split(jax.random.key(seed), 10)
    return {
        "tokens": draw_tokens(jax.random.fold_in(splits[9], 71), 0),
        "first_token_input": noise(splits[1], (SEQS_ALL, D), 1.0, 6.0, ((0, 2), (1, 8))),
        "forget_weight": draw_forget_weight(jax.random.fold_in(splits[9], 71), 0),
        "value_weight": noise(splits[3], (D, HW), (D // 16) ** -0.5, 0.375, ((1, 2),)),
        "query_weight": noise(splits[4], (D, HW), D ** -0.5, 0.09375, ((0, 8), (1, 2))),
        "output_gate_weight": noise(splits[5], (D, HW), D ** -0.5, 0.09375, ((0, 8), (1, 2))),
        "forget_bound_slack": draw_forget_bound_slack(jax.random.fold_in(splits[9], 71), 0),
        "additional_damping_exponent": draw_additional_damping_exponent(jax.random.fold_in(splits[9], 71), 0),
        "read_norm_scale": jnp.clip(1.0 + 0.18 * jax.random.normal(splits[8], (ATTENTION_SPAN,), jnp.float32), 0.1, 1.9),
    }


def reference(tokens, first_token_input, forget_weight, value_weight, query_weight, output_gate_weight, forget_bound_slack, additional_damping_exponent, read_norm_scale):

    def sequence_wise(couple_bundle):
        series_lines, segment_damping_exponent = couple_bundle
        forget = jnp.dot(series_lines, forget_weight, preferred_element_type=jnp.float32).astype(jnp.bfloat16)
        values = jnp.dot(series_lines, value_weight, preferred_element_type=jnp.float32).astype(jnp.bfloat16)
        valve_sampler_seeds = forget_bound_slack * jax.nn.sigmoid(-forget.astype(jnp.float32))
        damping_exponent = jnp.log1p(-valve_sampler_seeds) + jnp.repeat(segment_damping_exponent, ATTENTION_SPAN, axis=1)
        later_sum = jnp.cumsum(damping_exponent[::-1], axis=0)[::-1] - damping_exponent
        weighted = (valve_sampler_seeds * jnp.exp(later_sum)).astype(jnp.bfloat16)
        key_weights = weighted.astype(jnp.float32).reshape(LEN, HEADS, ATTENTION_SPAN)
        value_rows = values.astype(jnp.float32).reshape(LEN, HEADS, ATTENTION_SPAN)
        return jnp.einsum('lha,lhb->hab', key_weights, value_rows).astype(jnp.bfloat16)
    cache = lax.map(sequence_wise, (tokens, additional_damping_exponent))
    new_query = jnp.dot(first_token_input, query_weight, preferred_element_type=jnp.float32).astype(jnp.bfloat16)
    new_gate = jnp.dot(first_token_input, output_gate_weight, preferred_element_type=jnp.float32).astype(jnp.bfloat16)
    new_forget = jnp.dot(first_token_input, forget_weight, preferred_element_type=jnp.float32).astype(jnp.bfloat16)
    new_value = jnp.dot(first_token_input, value_weight, preferred_element_type=jnp.float32).astype(jnp.bfloat16)
    seq_count = first_token_input.shape[0]
    new_keys = (forget_bound_slack * jax.nn.sigmoid(-new_forget.astype(jnp.float32))).reshape(seq_count, HEADS, ATTENTION_SPAN)
    value_new = new_value.astype(jnp.float32).reshape(seq_count, HEADS, ATTENTION_SPAN)
    updated = (1.0 - new_keys)[..., None] * cache.astype(jnp.float32) + new_keys[..., None] * value_new[:, :, None, :]
    query_rows = new_query.astype(jnp.float32).reshape(seq_count, HEADS, ATTENTION_SPAN)
    read_sum = jnp.einsum('sha,shab->shb', query_rows, updated, precision=lax.Precision.HIGHEST)
    scaled = read_sum * lax.rsqrt(lax.optimization_barrier(jnp.mean(read_sum * read_sum, axis=-1, keepdims=True)) + 1e-06) * read_norm_scale
    first_read = (scaled.reshape(seq_count, HEADS * ATTENTION_SPAN) * jax.nn.silu(new_gate.astype(jnp.float32))).astype(jnp.bfloat16)
    return (cache, first_read)
```

```python
import functools

import jax
import jax.numpy as jnp
from jax import lax
from jax.experimental import pallas as pl
from jax.experimental.pallas import tpu as pltpu
from jax.sharding import PartitionSpec as P

F32 = jnp.float32
BF16 = jnp.bfloat16
GROUP_HEADS = 2
XROWS = 16


def kernel(
    dims,
    tokens,
    x_pad,
    qw,
    gw,
    wf,
    wv,
    slack,
    damp,
    scale,
    cache,
    first,
    seg,
    qw_s,
    gw_s,
    f_s,
    wk_s,
    v_s,
    nk_s,
    nv_s,
    tot,
    totr,
    later_s,
    qg,
    qgr,
    buf_a,
    rec_a,
    buf_b,
    rec_b,
    wt_s,
    rd,
    rdr,
    loc_sem,
    tok_ss,
    tok_rs,
    x_ss,
    x_rs,
    t_ss,
    t_rs,
    q_ss,
    q_rs,
    a_ss,
    a_rs,
    b_ss,
    b_rs,
    r_ss,
    r_rs,
):
    n, tp, seqs, length, groups, hd = dims
    hg = GROUP_HEADS
    width = hg * hd
    rows = seqs * length
    nz = n // 2
    own = hd // n
    g = pl.program_id(0)
    me = lax.axis_index("sp")
    tme = lax.axis_index("tp")
    y = lax.rem(me, 2)
    z = me // 2
    dp = tokens.shape[1]
    xw = x_pad.shape[1]

    def rcopy(src, dst, ss, rs, where):
        return pltpu.make_async_remote_copy(
            src_ref=src,
            dst_ref=dst,
            send_sem=ss,
            recv_sem=rs,
            device_id=where,
            device_id_type=pl.DeviceIdType.MESH,
        )

    gr = lax.axis_index("gr")

    def at_sp(p):
        return (gr, p, tme)

    def at_tp(t):
        return (gr, me, t)

    def up(d):
        return lax.rem(me + d, n)

    def seg_tok(t):
        return seg.at[pl.ds(0, rows), pl.ds(pl.multiple_of(t * dp, dp), dp)]

    def seg_x(p):
        return seg.at[pl.ds(rows, XROWS), pl.ds(pl.multiple_of(p * xw, xw), xw)]

    def tok_copy(d):
        return rcopy(tokens, seg_tok(tme), tok_ss.at[d - 1], tok_rs.at[d - 1], at_tp(lax.rem(tme + d, tp)))

    def x_copy(d):
        return rcopy(x_pad, seg_x(me), x_ss.at[d - 1], x_rs.at[d - 1], at_sp(up(d)))

    def local(k):
        src, dst = [(tokens, seg_tok(tme)), (x_pad, seg_x(me)), (qw, qw_s), (gw, gw_s)][k]
        return pltpu.make_async_copy(src, dst, loc_sem.at[k])

    def t_copy(k, d):
        return rcopy(tot.at[k], totr.at[k, d - 1], t_ss.at[k, d - 1], t_rs.at[k, d - 1], at_sp(up(d)))

    def q_copy(d):
        return rcopy(qg, qgr.at[d - 1], q_ss.at[d - 1], q_rs.at[d - 1], at_sp(up(d)))

    def a_copy(k):
        return rcopy(buf_a.at[k, 1 - y], rec_a.at[k], a_ss.at[k], a_rs.at[k], at_sp(me + 1 - 2 * y))

    def b_copy(k, d):
        there = lax.rem(z + d, nz)
        return rcopy(buf_b.at[k, there], rec_b.at[k, d - 1], b_ss.at[k, d - 1], b_rs.at[k, d - 1], at_sp(2 * there + y))

    def r_copy(k, d):
        return rcopy(rd.at[k], rdr.at[k, d - 1], r_ss.at[k, d - 1], r_rs.at[k, d - 1], at_sp(up(d)))

    @pl.when(g == 0)
    def _():
        local(0).start()
        local(1).start()
        barrier = pltpu.get_barrier_semaphore()
        for d in range(1, n):
            pl.semaphore_signal(barrier, inc=1, device_id=at_sp(up(d)), device_id_type=pl.DeviceIdType.MESH)
        for d in range(1, tp):
            pl.semaphore_signal(
                barrier, inc=1, device_id=at_tp(lax.rem(tme + d, tp)), device_id_type=pl.DeviceIdType.MESH
            )
        pl.semaphore_wait(barrier, n - 1 + tp - 1)
        for d in range(1, n):
            x_copy(d).start()
        for d in range(1, tp):
            tok_copy(d).start()
        local(2).start()
        local(3).start()
        local(0).wait()
        local(1).wait()
        for d in range(1, n):
            x_copy(d).wait_recv()

    for r in range(tp):
        if r > 0:

            @pl.when(g == 0)
            def _():
                tok_copy(tp - r).wait_recv()

        cut = pl.ds(pl.multiple_of(lax.rem(tme + r, tp) * dp, dp), dp)
        part = jnp.dot(seg[:, cut], wf[cut, :], preferred_element_type=F32)
        if r == 0:
            f_s[...] = part
        else:
            f_s[...] += part

    slot = lax.rem(g, 2)
    gap = slack[0]
    later_than = (
        lax.broadcasted_iota(jnp.int32, (length, length), 1) > lax.broadcasted_iota(jnp.int32, (length, length), 0)
    ).astype(BF16)
    for s in range(seqs):
        f = f_s[pl.ds(s * length, length), :].astype(BF16).astype(F32)
        keys = gap * jax.nn.sigmoid(-f)
        damping = damp[0, pl.ds(s * length, length), :]
        wide = jnp.concatenate([jnp.broadcast_to(damping[:, h : h + 1], (length, hd)) for h in range(hg)], axis=1)
        decay = jnp.log1p(-keys) + wide
        high = decay.astype(BF16)
        low = (decay - high.astype(F32)).astype(BF16)
        within = jnp.dot(later_than, high, preferred_element_type=F32) + jnp.dot(
            later_than, low, preferred_element_type=F32
        )
        wk_s[slot, pl.ds(s * length, length), :] = keys * jnp.exp(within)
        tot[g, pl.ds(s, 1), :] = within[0:1, :] + decay[0:1, :]
    for d in range(1, n):

        @pl.when(me + d >= n)
        def _():
            t_copy(g, d).start()

    nk_s[g] = gap * jax.nn.sigmoid(-f_s[pl.ds(rows, 8), :].astype(BF16).astype(F32))

    v = jnp.dot(seg[...], wv[...], preferred_element_type=F32).astype(BF16)
    v_s[slot] = v[:rows]
    nv_s[g] = v[rows:, :].astype(F32)

    @pl.when(g == 0)
    def _():
        local(2).wait()
        local(3).wait()
        xq = x_pad[...]
        qg[0:seqs, :] = jnp.dot(xq, qw_s[...], preferred_element_type=F32)[:seqs].astype(BF16)
        qg[seqs : 2 * seqs, :] = jnp.dot(xq, gw_s[...], preferred_element_type=F32)[:seqs].astype(BF16)
        for d in range(1, n):
            q_copy(d).start()

    def states(k):
        ks = lax.rem(k, 2)
        later_s[...] = jnp.zeros_like(later_s)
        for d in range(1, n):

            @pl.when(d > me)
            def _():
                t_copy(k, d).wait_recv()
                later_s[...] += totr[k, d - 1]

        faded = jnp.exp(later_s[...])
        for s in range(seqs):
            cut = pl.ds(s * length, length)
            w = (wk_s[ks, cut, :] * faded[s : s + 1, :]).astype(BF16)
            st = lax.dot_general(w, v_s[ks, cut, :], (((0,), (0,)), ((), ())), preferred_element_type=F32)
            for h in range(hg):
                block = st[h * hd : (h + 1) * hd, h * hd : (h + 1) * hd].astype(BF16)
                for p in range(n):
                    buf_a[k, p % 2, p // 2, s, h] = block[p * own : (p + 1) * own, :]
        a_copy(k).start()

    def pair(k):
        a_copy(k).wait_recv()
        buf_b[k] = (buf_a[k, y].astype(F32) + rec_a[k].astype(F32)).astype(BF16)
        for d in range(1, nz):
            b_copy(k, d).start()

    def query_gate(k):
        cut = pl.ds(pl.multiple_of(k * width, width), width)
        both = qg[:, cut].astype(F32)
        for d in range(1, n):
            both = both + qgr[d - 1, :, cut].astype(F32)
        return both.astype(BF16).astype(F32)

    def finish(k):
        total = buf_b[k, z].astype(F32)
        for d in range(1, nz):
            b_copy(k, d).wait_recv()
            total = total + rec_b[k, d - 1].astype(F32)
        kept = total.astype(BF16)
        q = query_gate(k)[:seqs]
        nk = nk_s[k, 0:seqs, :]
        fill = jnp.zeros((128 - 2 * seqs, width), F32)
        wt_s[...] = jnp.concatenate([q * (1.0 - nk), q * nk, fill], axis=0).T
        for h in range(hg):
            for s in range(seqs):
                cache[s, k * hg + h] = kept[s, h]
                mine = wt_s[pl.ds(pl.multiple_of(h * hd + me * own, own), own), :]
                old = jnp.sum(mine[:, s : s + 1] * kept[s, h].astype(F32), axis=0, keepdims=True)
                new = jnp.sum(
                    mine[:, seqs + s : seqs + s + 1] * nv_s[k, s : s + 1, h * hd : (h + 1) * hd], axis=0, keepdims=True
                )
                rd[k, s : s + 1, h * hd : (h + 1) * hd] = old + new
        for d in range(1, n):
            r_copy(k, d).start()

    def close(k):
        total = rd[k]
        for d in range(1, n):
            r_copy(k, d).wait_recv()
            total = total + rdr[k, d - 1]
        gate = query_gate(k)[seqs:]
        parts = []
        for h in range(hg):
            one = total[:, h * hd : (h + 1) * hd]
            parts.append(one * lax.rsqrt(jnp.mean(one * one, axis=-1, keepdims=True) + 1e-06) * scale[...])
        out = jnp.concatenate(parts, axis=1) * (gate * jax.nn.sigmoid(gate))
        first[:, pl.ds(pl.multiple_of(k * width, width), width)] = out.astype(BF16)

    def gathered():
        for d in range(1, n):
            q_copy(d).wait_recv()

    @pl.when(g >= 1)
    def _():
        states(g - 1)

    @pl.when(g >= 2)
    def _():
        pair(g - 2)

    if groups > 3:

        @pl.when(g == 3)
        def _():
            gathered()

        @pl.when(g >= 3)
        def _():
            finish(g - 3)

    @pl.when(g == groups - 1)
    def _():
        states(groups - 1)
        if groups <= 3:
            gathered()
        for k in range(max(groups - 2, 0), groups):
            pair(k)

        @pl.loop(max(groups - 3, 0), groups)
        def _(k):
            finish(k)

        @pl.loop(0, groups)
        def _(k):
            close(k)

        for d in range(1, n):
            x_copy(d).wait_send()
            q_copy(d).wait_send()
        for d in range(1, tp):
            tok_copy(d).wait_send()

        @pl.loop(0, groups)
        def _(k):
            a_copy(k).wait_send()
            for d in range(1, nz):
                b_copy(k, d).wait_send()
            for d in range(1, n):
                r_copy(k, d).wait_send()

                @pl.when(me + d >= n)
                def _():
                    t_copy(k, d).wait_send()


def per_device(
    tokens,
    first_token_input,
    forget_weight,
    value_weight,
    query_weight,
    output_gate_weight,
    forget_bound_slack,
    additional_damping_exponent,
    read_norm_scale,
):
    seqs, length, dp = tokens.shape
    hd = read_norm_scale.shape[0]
    heads = additional_damping_exponent.shape[2]
    n, tp = lax.axis_size("sp"), lax.axis_size("tp")
    hg = GROUP_HEADS
    groups = heads // hg
    width = hg * hd
    channels = heads * hd
    rows = seqs * length
    features = forget_weight.shape[0]
    xw = first_token_input.shape[1]
    own = hd // n
    nz = n // 2
    x_pad = jnp.pad(first_token_input, ((0, XROWS - seqs), (0, 0)))
    damp = additional_damping_exponent.reshape(rows, groups, hg).transpose(1, 0, 2)
    slack = forget_bound_slack.reshape(groups, 1, width)
    anywhere = pl.BlockSpec(memory_space=pl.ANY)
    whole = pl.BlockSpec(memory_space=pltpu.VMEM)
    dma = pltpu.SemaphoreType.DMA
    return pl.pallas_call(
        functools.partial(kernel, (n, tp, seqs, length, groups, hd)),
        grid=(groups,),
        out_shape=(
            jax.ShapeDtypeStruct((seqs, heads, own, hd), BF16),
            jax.ShapeDtypeStruct((seqs, channels), BF16),
        ),
        in_specs=[
            anywhere,
            whole,
            anywhere,
            anywhere,
            pl.BlockSpec((features, width), lambda g: (0, g)),
            pl.BlockSpec((features, width), lambda g: (0, g)),
            pl.BlockSpec((1, 1, width), lambda g: (g, 0, 0)),
            pl.BlockSpec((1, rows, hg), lambda g: (g, 0, 0)),
            whole,
        ],
        out_specs=(whole, whole),
        scratch_shapes=[
            pltpu.VMEM((rows + XROWS, features), BF16),
            pltpu.VMEM((xw, channels), BF16),
            pltpu.VMEM((xw, channels), BF16),
            pltpu.VMEM((rows + XROWS, width), F32),
            pltpu.VMEM((2, rows, width), F32),
            pltpu.VMEM((2, rows, width), BF16),
            pltpu.VMEM((groups, 8, width), F32),
            pltpu.VMEM((groups, XROWS, width), F32),
            pltpu.VMEM((groups, seqs, width), F32),
            pltpu.VMEM((groups, n - 1, seqs, width), F32),
            pltpu.VMEM((seqs, width), F32),
            pltpu.VMEM((2 * seqs, channels), BF16),
            pltpu.VMEM((n - 1, 2 * seqs, channels), BF16),
            pltpu.VMEM((groups, 2, nz, seqs, hg, own, hd), BF16),
            pltpu.VMEM((groups, nz, seqs, hg, own, hd), BF16),
            pltpu.VMEM((groups, nz, seqs, hg, own, hd), BF16),
            pltpu.VMEM((groups, nz - 1, seqs, hg, own, hd), BF16),
            pltpu.VMEM((width, 128), F32),
            pltpu.VMEM((groups, seqs, width), F32),
            pltpu.VMEM((groups, n - 1, seqs, width), F32),
            dma((4,)),
            dma((tp - 1,)),
            dma((tp - 1,)),
            dma((n - 1,)),
            dma((n - 1,)),
            dma((groups, n - 1)),
            dma((groups, n - 1)),
            dma((n - 1,)),
            dma((n - 1,)),
            dma((groups,)),
            dma((groups,)),
            dma((groups, nz - 1)),
            dma((groups, nz - 1)),
            dma((groups, n - 1)),
            dma((groups, n - 1)),
        ],
        compiler_params=pltpu.CompilerParams(
            collective_id=0,
            has_side_effects=True,
            dimension_semantics=("arbitrary",),
            vmem_limit_bytes=60 * 1024 * 1024,
        ),
    )(
        tokens.reshape(rows, dp),
        x_pad,
        query_weight,
        output_gate_weight,
        forget_weight,
        value_weight,
        slack,
        damp,
        read_norm_scale.reshape(1, hd),
    )


def solution(mesh):
    placed = (
        P("gr", "sp", "tp"),
        P("gr", "sp"),
        P(None, "tp"),
        P(None, "tp"),
        P("sp", "tp"),
        P("sp", "tp"),
        P("tp"),
        P("gr", "sp", "tp"),
        P(),
    )
    return jax.shard_map(
        per_device,
        mesh=mesh,
        in_specs=placed,
        out_specs=(P("gr", "tp", "sp", None), P("gr", "tp")),
        check_vma=False,
    )
```

```python
import functools

import jax
import jax.numpy as jnp
from jax import lax
from jax.experimental import pallas as pl
from jax.experimental.pallas import tpu as pltpu
from jax.sharding import PartitionSpec as P

F32 = jnp.float32
BF16 = jnp.bfloat16
GROUP_HEADS = 2
XROWS = 16


def kernel(
    dims,
    tokens,
    x_pad,
    qw,
    gw,
    wf,
    wv,
    slack,
    damp,
    scale,
    cache,
    first,
    seg,
    qw_s,
    gw_s,
    f_s,
    wk_s,
    v_s,
    nk_s,
    nv_s,
    tot,
    totr,
    later_s,
    qg,
    qgr,
    buf_a,
    rec_a,
    buf_b,
    rec_b,
    wt_s,
    rd,
    rdr,
    loc_sem,
    tok_ss,
    tok_rs,
    x_ss,
    x_rs,
    t_ss,
    t_rs,
    q_ss,
    q_rs,
    a_ss,
    a_rs,
    b_ss,
    b_rs,
    r_ss,
    r_rs,
):
    n, tp, seqs, length, groups, hd = dims
    hg = GROUP_HEADS
    width = hg * hd
    rows = seqs * length
    nz = n // 2
    own = hd // n
    g = pl.program_id(0)
    me = lax.axis_index("sp")
    tme = lax.axis_index("tp")
    y = lax.rem(me, 2)
    z = me // 2
    dp = tokens.shape[1]
    xw = x_pad.shape[1]

    def rcopy(src, dst, ss, rs, where):
        return pltpu.make_async_remote_copy(
            src_ref=src,
            dst_ref=dst,
            send_sem=ss,
            recv_sem=rs,
            device_id=where,
            device_id_type=pl.DeviceIdType.MESH,
        )

    gr = lax.axis_index("gr")

    def at_sp(p):
        return (gr, p, tme)

    def at_tp(t):
        return (gr, me, t)

    def up(d):
        return lax.rem(me + d, n)

    def seg_tok(t):
        return seg.at[pl.ds(0, rows), pl.ds(pl.multiple_of(t * dp, dp), dp)]

    def seg_x(p):
        return seg.at[pl.ds(rows, XROWS), pl.ds(pl.multiple_of(p * xw, xw), xw)]

    def tok_copy(d):
        return rcopy(tokens, seg_tok(tme), tok_ss.at[d - 1], tok_rs.at[d - 1], at_tp(lax.rem(tme + d, tp)))

    def x_copy(d):
        return rcopy(x_pad, seg_x(me), x_ss.at[d - 1], x_rs.at[d - 1], at_sp(up(d)))

    def local(k):
        src, dst = [(tokens, seg_tok(tme)), (x_pad, seg_x(me)), (qw, qw_s), (gw, gw_s)][k]
        return pltpu.make_async_copy(src, dst, loc_sem.at[k])

    def t_copy(k, d):
        return rcopy(tot.at[k], totr.at[k, d - 1], t_ss.at[k, d - 1], t_rs.at[k, d - 1], at_sp(up(d)))

    def q_copy(d):
        return rcopy(qg, qgr.at[d - 1], q_ss.at[d - 1], q_rs.at[d - 1], at_sp(up(d)))

    def a_copy(k):
        return rcopy(buf_a.at[k, 1 - y], rec_a.at[k], a_ss.at[k], a_rs.at[k], at_sp(me + 1 - 2 * y))

    def b_copy(k, d):
        there = lax.rem(z + d, nz)
        return rcopy(buf_b.at[k, there], rec_b.at[k, d - 1], b_ss.at[k, d - 1], b_rs.at[k, d - 1], at_sp(2 * there + y))

    def r_copy(k, d):
        return rcopy(rd.at[k], rdr.at[k, d - 1], r_ss.at[k, d - 1], r_rs.at[k, d - 1], at_sp(up(d)))

    @pl.when(g == 0)
    def _():
        local(0).start()
        local(1).start()
        barrier = pltpu.get_barrier_semaphore()
        for d in range(1, n):
            pl.semaphore_signal(barrier, inc=1, device_id=at_sp(up(d)), device_id_type=pl.DeviceIdType.MESH)
        for d in range(1, tp):
            pl.semaphore_signal(
                barrier, inc=1, device_id=at_tp(lax.rem(tme + d, tp)), device_id_type=pl.DeviceIdType.MESH
            )
        pl.semaphore_wait(barrier, n - 1 + tp - 1)
        for d in range(1, n):
            x_copy(d).start()
        for d in range(1, tp):
            tok_copy(d).start()
        local(2).start()
        local(3).start()
        local(0).wait()
        local(1).wait()
        for d in range(1, n):
            x_copy(d).wait_recv()

    for r in range(tp):
        if r > 0:

            @pl.when(g == 0)
            def _():
                tok_copy(tp - r).wait_recv()

        cut = pl.ds(pl.multiple_of(lax.rem(tme + r, tp) * dp, dp), dp)
        both = jnp.concatenate([wf[cut, :], wv[cut, :]], axis=1)
        part = jnp.dot(seg[:, cut], both, preferred_element_type=F32)
        if r == 0:
            f_s[...] = part
        else:
            f_s[...] += part

    slot = lax.rem(g, 2)
    gap = slack[0]
    later_than = (
        lax.broadcasted_iota(jnp.int32, (length, length), 1) > lax.broadcasted_iota(jnp.int32, (length, length), 0)
    ).astype(BF16)
    for s in range(seqs):
        f = f_s[pl.ds(s * length, length), :width].astype(BF16).astype(F32)
        keys = gap * jax.nn.sigmoid(-f)
        damping = damp[0, pl.ds(s * length, length), :]
        wide = jnp.concatenate([jnp.broadcast_to(damping[:, h : h + 1], (length, hd)) for h in range(hg)], axis=1)
        decay = jnp.log1p(-keys) + wide
        high = decay.astype(BF16)
        low = (decay - high.astype(F32)).astype(BF16)
        within = jnp.dot(later_than, high, preferred_element_type=F32) + jnp.dot(
            later_than, low, preferred_element_type=F32
        )
        wk_s[slot, pl.ds(s * length, length), :] = keys * jnp.exp(within)
        tot[g, pl.ds(s, 1), :] = within[0:1, :] + decay[0:1, :]
    for d in range(1, n):

        @pl.when(me + d >= n)
        def _():
            t_copy(g, d).start()

    nk_s[g] = gap * jax.nn.sigmoid(-f_s[pl.ds(rows, 8), :width].astype(BF16).astype(F32))

    v = f_s[:, width:].astype(BF16)
    v_s[slot] = v[:rows]
    nv_s[g] = v[rows:, :].astype(F32)

    @pl.when(g == 0)
    def _():
        local(2).wait()
        local(3).wait()
        xq = x_pad[...]
        qg[0:seqs, :] = jnp.dot(xq, qw_s[...], preferred_element_type=F32)[:seqs].astype(BF16)
        qg[seqs : 2 * seqs, :] = jnp.dot(xq, gw_s[...], preferred_element_type=F32)[:seqs].astype(BF16)
        for d in range(1, n):
            q_copy(d).start()

    def states(k):
        ks = lax.rem(k, 2)
        later_s[...] = jnp.zeros_like(later_s)
        for d in range(1, n):

            @pl.when(d > me)
            def _():
                t_copy(k, d).wait_recv()
                later_s[...] += totr[k, d - 1]

        faded = jnp.exp(later_s[...])
        for s in range(seqs):
            cut = pl.ds(s * length, length)
            w = (wk_s[ks, cut, :] * faded[s : s + 1, :]).astype(BF16)
            st = lax.dot_general(w, v_s[ks, cut, :], (((0,), (0,)), ((), ())), preferred_element_type=F32)
            for h in range(hg):
                block = st[h * hd : (h + 1) * hd, h * hd : (h + 1) * hd].astype(BF16)
                for p in range(n):
                    buf_a[k, p % 2, p // 2, s, h] = block[p * own : (p + 1) * own, :]
        a_copy(k).start()

    def pair(k):
        a_copy(k).wait_recv()
        buf_b[k] = (buf_a[k, y].astype(F32) + rec_a[k].astype(F32)).astype(BF16)
        for d in range(1, nz):
            b_copy(k, d).start()

    def query_gate(k):
        cut = pl.ds(pl.multiple_of(k * width, width), width)
        both = qg[:, cut].astype(F32)
        for d in range(1, n):
            both = both + qgr[d - 1, :, cut].astype(F32)
        return both.astype(BF16).astype(F32)

    def finish(k):
        total = buf_b[k, z].astype(F32)
        for d in range(1, nz):
            b_copy(k, d).wait_recv()
            total = total + rec_b[k, d - 1].astype(F32)
        kept = total.astype(BF16)
        q = query_gate(k)[:seqs]
        nk = nk_s[k, 0:seqs, :]
        fill = jnp.zeros((128 - 2 * seqs, width), F32)
        wt_s[...] = jnp.concatenate([q * (1.0 - nk), q * nk, fill], axis=0).T
        for h in range(hg):
            for s in range(seqs):
                cache[s, k * hg + h] = kept[s, h]
                mine = wt_s[pl.ds(pl.multiple_of(h * hd + me * own, own), own), :]
                old = jnp.sum(mine[:, s : s + 1] * kept[s, h].astype(F32), axis=0, keepdims=True)
                new = jnp.sum(
                    mine[:, seqs + s : seqs + s + 1] * nv_s[k, s : s + 1, h * hd : (h + 1) * hd], axis=0, keepdims=True
                )
                rd[k, s : s + 1, h * hd : (h + 1) * hd] = old + new
        for d in range(1, n):
            r_copy(k, d).start()

    def close(k):
        total = rd[k]
        for d in range(1, n):
            r_copy(k, d).wait_recv()
            total = total + rdr[k, d - 1]
        gate = query_gate(k)[seqs:]
        parts = []
        for h in range(hg):
            one = total[:, h * hd : (h + 1) * hd]
            parts.append(one * lax.rsqrt(jnp.mean(one * one, axis=-1, keepdims=True) + 1e-06) * scale[...])
        out = jnp.concatenate(parts, axis=1) * (gate * jax.nn.sigmoid(gate))
        first[:, pl.ds(pl.multiple_of(k * width, width), width)] = out.astype(BF16)

    def gathered():
        for d in range(1, n):
            q_copy(d).wait_recv()

    @pl.when(g >= 1)
    def _():
        states(g - 1)

    @pl.when(g >= 2)
    def _():
        pair(g - 2)

    if groups > 3:

        @pl.when(g == 3)
        def _():
            gathered()

        @pl.when(g >= 3)
        def _():
            finish(g - 3)

    @pl.when(g == groups - 1)
    def _():
        states(groups - 1)
        if groups <= 3:
            gathered()
        if groups >= 2:
            pair(groups - 2)
        if groups >= 3:
            finish(groups - 3)
        pair(groups - 1)
        if groups >= 2:
            finish(groups - 2)
        finish(groups - 1)

        @pl.loop(0, groups)
        def _(k):
            close(k)

        for d in range(1, n):
            x_copy(d).wait_send()
            q_copy(d).wait_send()
        for d in range(1, tp):
            tok_copy(d).wait_send()

        @pl.loop(0, groups)
        def _(k):
            a_copy(k).wait_send()
            for d in range(1, nz):
                b_copy(k, d).wait_send()
            for d in range(1, n):
                r_copy(k, d).wait_send()

                @pl.when(me + d >= n)
                def _():
                    t_copy(k, d).wait_send()


def per_device(
    tokens,
    first_token_input,
    forget_weight,
    value_weight,
    query_weight,
    output_gate_weight,
    forget_bound_slack,
    additional_damping_exponent,
    read_norm_scale,
):
    seqs, length, dp = tokens.shape
    hd = read_norm_scale.shape[0]
    heads = additional_damping_exponent.shape[2]
    n, tp = lax.axis_size("sp"), lax.axis_size("tp")
    hg = GROUP_HEADS
    groups = heads // hg
    width = hg * hd
    channels = heads * hd
    rows = seqs * length
    features = forget_weight.shape[0]
    xw = first_token_input.shape[1]
    own = hd // n
    nz = n // 2
    x_pad = jnp.pad(first_token_input, ((0, XROWS - seqs), (0, 0)))
    damp = additional_damping_exponent.reshape(rows, groups, hg).transpose(1, 0, 2)
    slack = forget_bound_slack.reshape(groups, 1, width)
    anywhere = pl.BlockSpec(memory_space=pl.ANY)
    whole = pl.BlockSpec(memory_space=pltpu.VMEM)
    dma = pltpu.SemaphoreType.DMA
    return pl.pallas_call(
        functools.partial(kernel, (n, tp, seqs, length, groups, hd)),
        grid=(groups,),
        out_shape=(
            jax.ShapeDtypeStruct((seqs, heads, own, hd), BF16),
            jax.ShapeDtypeStruct((seqs, channels), BF16),
        ),
        in_specs=[
            anywhere,
            whole,
            anywhere,
            anywhere,
            pl.BlockSpec((features, width), lambda g: (0, g)),
            pl.BlockSpec((features, width), lambda g: (0, g)),
            pl.BlockSpec((1, 1, width), lambda g: (g, 0, 0)),
            pl.BlockSpec((1, rows, hg), lambda g: (g, 0, 0)),
            whole,
        ],
        out_specs=(whole, whole),
        scratch_shapes=[
            pltpu.VMEM((rows + XROWS, features), BF16),
            pltpu.VMEM((xw, channels), BF16),
            pltpu.VMEM((xw, channels), BF16),
            pltpu.VMEM((rows + XROWS, 2 * width), F32),
            pltpu.VMEM((2, rows, width), F32),
            pltpu.VMEM((2, rows, width), BF16),
            pltpu.VMEM((groups, 8, width), F32),
            pltpu.VMEM((groups, XROWS, width), F32),
            pltpu.VMEM((groups, seqs, width), F32),
            pltpu.VMEM((groups, n - 1, seqs, width), F32),
            pltpu.VMEM((seqs, width), F32),
            pltpu.VMEM((2 * seqs, channels), BF16),
            pltpu.VMEM((n - 1, 2 * seqs, channels), BF16),
            pltpu.VMEM((groups, 2, nz, seqs, hg, own, hd), BF16),
            pltpu.VMEM((groups, nz, seqs, hg, own, hd), BF16),
            pltpu.VMEM((groups, nz, seqs, hg, own, hd), BF16),
            pltpu.VMEM((groups, nz - 1, seqs, hg, own, hd), BF16),
            pltpu.VMEM((width, 128), F32),
            pltpu.VMEM((groups, seqs, width), F32),
            pltpu.VMEM((groups, n - 1, seqs, width), F32),
            dma((4,)),
            dma((tp - 1,)),
            dma((tp - 1,)),
            dma((n - 1,)),
            dma((n - 1,)),
            dma((groups, n - 1)),
            dma((groups, n - 1)),
            dma((n - 1,)),
            dma((n - 1,)),
            dma((groups,)),
            dma((groups,)),
            dma((groups, nz - 1)),
            dma((groups, nz - 1)),
            dma((groups, n - 1)),
            dma((groups, n - 1)),
        ],
        compiler_params=pltpu.CompilerParams(
            collective_id=0,
            has_side_effects=True,
            dimension_semantics=("arbitrary",),
            vmem_limit_bytes=60 * 1024 * 1024,
        ),
    )(
        tokens.reshape(rows, dp),
        x_pad,
        query_weight,
        output_gate_weight,
        forget_weight,
        value_weight,
        slack,
        damp,
        read_norm_scale.reshape(1, hd),
    )


def solution(mesh):
    placed = (
        P("gr", "sp", "tp"),
        P("gr", "sp"),
        P(None, "tp"),
        P(None, "tp"),
        P("sp", "tp"),
        P("sp", "tp"),
        P("tp"),
        P("gr", "sp", "tp"),
        P(),
    )
    return jax.shard_map(
        per_device,
        mesh=mesh,
        in_specs=placed,
        out_specs=(P("gr", "tp", "sp", None), P("gr", "tp")),
        check_vma=False,
    )
```
